32 devices in a mesh: sp: 16 (over z, y, x), tp: 2 (over core).
Axes of the slice: x: 2, y: 2, z: 4, core: 2. Of those that a mesh axis runs over, the one named last changes fastest.
Arguments:
- residual: bfloat16 [2048, 2048], P('sp'), may hold values from -6 to 6
- query_nope: bfloat16 [2048, 8, 128], P('sp', 'tp'), may hold values from -6 to 6
- query_rope: bfloat16 [2048, 8, 64], P('sp', 'tp'), may hold values from -64 to 64
- latent: bfloat16 [2048, 256], P('sp'), may hold values from -6 to 6
- rope_key: bfloat16 [2048, 64], P('sp'), may hold values from -64 to 64
- kv_gain: bfloat16 [256], replicated, may hold values from 0.099609375 to 1.8984375
- key_up: bfloat16 [256, 8, 128], replicated, may hold values from -0.375 to 0.375
- value_up: bfloat16 [256, 8, 128], replicated, may hold values from -0.375 to 0.375
- out_weight: bfloat16 [1024, 2048], P('tp'), may hold values from -0.1875 to 0.1875
- post_gain: bfloat16 [2048], replicated, may hold values from 0.099609375 to 1.8984375
- pre_gain: bfloat16 [2048], replicated, may hold values from 0.099609375 to 1.8984375
- ffn_gain: bfloat16 [2048], replicated, may hold values from 0.099609375 to 1.8984375
- up_value: bfloat16 [2048, 5632], P('sp', 'tp'), may hold values from -0.125 to 0.125
- up_gate: bfloat16 [2048, 5632], P('sp', 'tp'), may hold values from -0.125 to 0.125
- conv_value: bfloat16 [3, 5632], replicated, may hold values from -3.5 to 3.5
- conv_gate: bfloat16 [3, 5632], replicated, may hold values from -3.5 to 3.5
- down_weight: bfloat16 [5632, 2048], P('tp', 'sp'), may hold values from -0.078125 to 0.078125
Outputs:
- layer_out: bfloat16 [2048, 2048], P(('sp', 'tp'))
The draws below stay inside these ranges and needn't reach their ends.
All inputs are finite; a program needn't handle non-finite values.
Results may differ from the reference program's by a relative error of at most 0.02.
Values may be sent and summed in bfloat16 or wider, within the bound.
No kernel may reach another device: no remote copies, remote signals or barrier semaphores. Data moves between devices by JAX's collectives and lax.ppermute only.
A program may use at most 128 MiB of HBM per device.

```python
import jax
import jax.numpy as jnp
from jax import lax

D = 2048
HEADS = 8
NOPE = 128
ROPE = 64
VD = 128
KV = 256
FF = 5632
GRID = 64
TOKENS = 2048
N_TP = 2


def drawn_pair(key):
    folded = jax.random.fold_in(key, 41)
    query_key, rope_seed = jax.random.split(folded, 2)
    queries = jax.random.normal(query_key, (TOKENS, HEADS, ROPE), jnp.float32)
    rope_keys = jax.random.normal(rope_seed, (TOKENS, ROPE), jnp.float32)
    return (jnp.clip(queries, -64.0, 64.0), jnp.clip(rope_keys, -64.0, 64.0))


def draw_query_rope(key, part):
    return drawn_pair(key)[0].astype(jnp.bfloat16)


def draw_rope_key(key, part):
    return drawn_pair(key)[1].astype(jnp.bfloat16)


def level_of(key, shape, cuts, smallest, top_value):
    loudness = 1.0
    for dim, parts in cuts:
        draws = jax.random.uniform(jax.random.fold_in(jax.random.fold_in(key, 6), dim), (parts,), jnp.float32, smallest / len(cuts), top_value / len(cuts))
        loudness = loudness * jnp.repeat(jnp.exp(draws), shape[dim] // parts).reshape((-1,) + (1,) * (len(shape) - 1 - dim))
    return loudness


def bell_draw(rng, dims, scale, most, cuts=(), held_as=jnp.bfloat16):
    entries = scale * jax.random.normal(rng, dims, jnp.float32)
    if cuts:
        entries = entries * level_of(rng, dims, cuts, -0.22, 0.18)
    return jnp.clip(entries, -most, most).astype(held_as)


def setup_inputs(seed: int = 0) -> dict:
    arg_keys = jax.random.split(jax.random.key(seed), 18)
    return {
        "residual": bell_draw(arg_keys[0], (TOKENS, D), 1.0, 6.0, ((0, 16),)),
        "query_nope": bell_draw(arg_keys[1], (TOKENS, HEADS, NOPE), 1.0, 6.0, ((0, 16), (1, 2))),
        "query_rope": draw_query_rope(jax.random.fold_in(arg_keys[17], 71), 0),
        "latent": bell_draw(arg_keys[3], (TOKENS, KV), 1.0, 6.0, ((0, 16),)),
        "rope_key": draw_rope_key(jax.random.fold_in(arg_keys[17], 71), 0),
        "kv_gain": jnp.clip(1.0 + 0.18 * jax.random.normal(arg_keys[5], (KV,), jnp.float32), 0.099609375, 1.8984375).astype(jnp.bfloat16),
        "key_up": bell_draw(arg_keys[6], (KV, HEADS, NOPE), KV ** -0.5, 0.375),
        "value_up": bell_draw(arg_keys[7], (KV, HEADS, VD), KV ** -0.5, 0.375),
        "out_weight": bell_draw(arg_keys[8], (HEADS * VD, D), (HEADS * VD) ** -0.5, 0.1875, ((0, 2),)),
        "post_gain": jnp.clip(1.0 + 0.18 * jax.random.normal(arg_keys[9], (D,), jnp.float32), 0.099609375, 1.8984375).astype(jnp.bfloat16),
        "pre_gain": jnp.clip(1.0 + 0.18 * jax.random.normal(arg_keys[10], (D,), jnp.float32), 0.099609375, 1.8984375).astype(jnp.bfloat16),
        "ffn_gain": jnp.clip(1.0 + 0.18 * jax.random.normal(arg_keys[11], (D,), jnp.float32), 0.099609375, 1.8984375).astype(jnp.bfloat16),
        "up_value": bell_draw(arg_keys[12], (D, FF), D ** -0.5, 0.125, ((0, 16), (1, 2))),
        "up_gate": bell_draw(arg_keys[13], (D, FF), D ** -0.5, 0.125, ((0, 16), (1, 2))),
        "conv_value": bell_draw(arg_keys[14], (3, FF), 3 ** -0.5, 3.5),
        "conv_gate": bell_draw(arg_keys[15], (3, FF), 3 ** -0.5, 3.5),
        "down_weight": bell_draw(arg_keys[16], (FF, D), FF ** -0.5, 0.078125, ((0, 2), (1, 16))),
    }


epsilon = 1e-06
rope_base = 10000.0

def rms_norm(values, gain):
    return values * lax.rsqrt(lax.optimization_barrier(jnp.mean(values * values, axis=-1, keepdims=True)) + epsilon) * gain.astype(jnp.float32)

def widened(values):
    return lax.optimization_barrier(values.astype(jnp.bfloat16)).astype(jnp.float32)

def rotate(values, positions):
    pair_count = values.shape[-1] // 4
    frequency = rope_base ** (-jnp.arange(pair_count, dtype=jnp.float32) / pair_count)
    grid_rows = (positions // GRID).astype(jnp.float32)
    grid_cols = (positions % GRID).astype(jnp.float32)
    angles = jnp.stack([grid_rows, grid_cols], axis=-1)[:, :, None] * frequency
    table_shape = (angles.shape[0],) + (1,) * (values.ndim - 2) + angles.shape[1:]
    cosine = jnp.cos(angles).reshape(table_shape)
    sine = jnp.sin(angles).reshape(table_shape)
    halves = values.reshape(values.shape[:-1] + (2, 2, pair_count))
    leading = halves[..., 0, :]
    trailing = halves[..., 1, :]
    turned = jnp.stack([leading * cosine - trailing * sine, trailing * cosine + leading * sine], axis=-2)
    return turned.reshape(values.shape)

def reference(residual, query_nope, query_rope, latent, rope_key, kv_gain, key_up, value_up, out_weight, post_gain, pre_gain, ffn_gain, up_value, up_gate, conv_value, conv_gate, down_weight):
    token_count = residual.shape[0]
    positions = jnp.arange(token_count, dtype=jnp.int32)
    score_scale = (NOPE + ROPE) ** (-0.5)
    normed_wide = widened(rms_norm(latent.astype(jnp.float32), kv_gain))
    keys_nope = widened(jnp.einsum('nc,chd->nhd', normed_wide, key_up.astype(jnp.float32)))
    values_all = widened(jnp.einsum('nc,chd->nhd', normed_wide, value_up.astype(jnp.float32)))
    key_turn = widened(rotate(rope_key.astype(jnp.float32), positions))
    query_turn = widened(rotate(query_rope.astype(jnp.float32), positions))
    keys_all = jnp.concatenate([keys_nope, jnp.broadcast_to(key_turn[:, None, :], (token_count, HEADS, ROPE))], axis=-1)
    queries = jnp.concatenate([query_nope.astype(jnp.float32), query_turn], axis=-1)
    block_size = min(512, token_count)
    query_blocks = queries.reshape(token_count // block_size, block_size, HEADS, NOPE + ROPE)

    def attend_block(query_block):
        scores = jnp.einsum('qhd,khd->hqk', query_block, keys_all) * score_scale
        row_max = lax.optimization_barrier(jnp.max(scores, axis=-1, keepdims=True))
        weights = jnp.exp(scores - row_max)
        totals = lax.optimization_barrier(jnp.sum(weights, axis=-1))
        mixed = jnp.einsum('hqk,khd->qhd', widened(weights), values_all)
        return (mixed / jnp.transpose(totals)[:, :, None]).astype(jnp.bfloat16)
    attended = lax.map(attend_block, query_blocks).reshape(token_count, HEADS * VD)
    group_width = HEADS * VD // N_TP

    def add_heads(running, group_id):
        block_rows = lax.dynamic_slice_in_dim(attended, group_id * group_width, group_width, 1)
        weight_rows = lax.dynamic_slice_in_dim(out_weight, group_id * group_width, group_width, 0)
        partial_value = jnp.dot(block_rows, weight_rows, preferred_element_type=jnp.float32)
        return (running + widened(partial_value), None)
    summed = lax.scan(add_heads, jnp.zeros((token_count, D), jnp.float32), jnp.arange(N_TP, dtype=jnp.int32))[0]
    stream_wide = widened(residual.astype(jnp.float32) + rms_norm(widened(summed), post_gain))
    inputs = rms_norm(stream_wide, pre_gain).astype(jnp.bfloat16)
    value_rows = widened(jnp.dot(inputs, up_value, preferred_element_type=jnp.float32))
    gate_rows = widened(jnp.dot(inputs, up_gate, preferred_element_type=jnp.float32))

    def convolve(rows_wide, conv_taps):
        padded = jnp.pad(rows_wide, ((1, 1), (0, 0)))
        return padded[:-2] * conv_taps[0] + padded[1:-1] * conv_taps[1] + padded[2:] * conv_taps[2]
    value_conv = convolve(value_rows, conv_value.astype(jnp.float32))
    gate_conv = convolve(gate_rows, conv_gate.astype(jnp.float32))
    hidden = (jax.nn.silu(gate_conv) * value_conv).astype(jnp.bfloat16)
    ff_width = FF // N_TP

    def add_units(running, group_id):
        block_rows = lax.dynamic_slice_in_dim(hidden, group_id * ff_width, ff_width, 1)
        weight_rows = lax.dynamic_slice_in_dim(down_weight, group_id * ff_width, ff_width, 0)
        partial_value = jnp.dot(block_rows, weight_rows, preferred_element_type=jnp.float32)
        return (running + widened(partial_value), None)
    projected = lax.scan(add_units, jnp.zeros((token_count, D), jnp.float32), jnp.arange(N_TP, dtype=jnp.int32))[0]
    return (stream_wide + rms_norm(widened(projected), ffn_gain)).astype(jnp.bfloat16)
```

```python
import jax
import jax.numpy as jnp
import numpy as np
from jax import lax
from jax.experimental import pallas as pl
from jax.experimental.pallas import tpu as pltpu
from jax.sharding import Mesh
from jax.sharding import PartitionSpec as P

BF16, F32 = jnp.bfloat16, jnp.float32
LOG2E = 1.4426950408889634
ATTEND_ROWS = 128

GRID = 64


epsilon = 1e-06
rope_base = 10000.0


def extended(x, sides, width):
    for axis, dim in sides:
        size, length = (lax.axis_size(axis), x.shape[dim])
        up = [(i, (i + 1) % size) for i in range(size - 1)]
        down = [(j, i) for i, j in up]
        last = lax.slice_in_dim(x, length - width, length, axis=dim)
        initial = lax.slice_in_dim(x, 0, width, axis=dim)
        before = lax.ppermute(last, axis, up)
        after = lax.ppermute(initial, axis, down)
        x = jnp.concatenate([before, x, after], axis=dim)
    return x


def rms_norm(values, gain):
    return (
        values
        * lax.rsqrt(jnp.mean(values * values, axis=-1, keepdims=True) + epsilon)
        * gain.astype(jnp.float32)
    )


def widened(values):
    return lax.optimization_barrier(values.astype(jnp.bfloat16)).astype(jnp.float32)


def rotate(values, positions):
    pair_count = values.shape[-1] // 4
    frequency = rope_base ** (-jnp.arange(pair_count, dtype=jnp.float32) / pair_count)
    grid_rows = (positions // GRID).astype(jnp.float32)
    grid_cols = (positions % GRID).astype(jnp.float32)
    angles = jnp.stack([grid_rows, grid_cols], axis=-1)[:, :, None] * frequency
    table_shape = (angles.shape[0],) + (1,) * (values.ndim - 2) + angles.shape[1:]
    cosine = jnp.cos(angles).reshape(table_shape)
    sine = jnp.sin(angles).reshape(table_shape)
    halves = values.reshape(values.shape[:-1] + (2, 2, pair_count))
    leading = halves[..., 0, :]
    trailing = halves[..., 1, :]
    turned = jnp.stack(
        [leading * cosine - trailing * sine, trailing * cosine + leading * sine], axis=-2
    )
    return turned.reshape(values.shape)


def body(
    residual,
    query_nope,
    query_rope,
    latent,
    rope_key,
    kv_gain,
    key_up,
    value_up,
    out_weight,
    post_gain,
    pre_gain,
    ffn_gain,
    up_value,
    up_gate,
    conv_value,
    conv_gate,
    down_weight,
):
    tok_rows = residual.shape[0]
    heads_dev = query_nope.shape[1]
    value_width = value_up.shape[2]
    tp_index = lax.axis_index("tp")
    positions = lax.axis_index("sp") * tok_rows + jnp.arange(tok_rows, dtype=jnp.int32)
    score_scale = (query_nope.shape[2] + query_rope.shape[2]) ** (-0.5)
    normed = rms_norm(latent.astype(jnp.float32), kv_gain).astype(jnp.bfloat16)
    key_turn = rotate(rope_key.astype(jnp.float32), positions).astype(jnp.bfloat16)
    query_turn = rotate(query_rope.astype(jnp.float32), positions).astype(jnp.bfloat16)
    key_local = lax.dynamic_slice_in_dim(key_up, tp_index * heads_dev, heads_dev, 1)
    value_local = lax.dynamic_slice_in_dim(value_up, tp_index * heads_dev, heads_dev, 1)
    pieces = (
        lax.all_gather(normed, "sp", axis=0, tiled=True),
        lax.all_gather(key_turn, "sp", axis=0, tiled=True),
    )
    keys_nope = jnp.einsum(
        "nc,chd->nhd", pieces[0], key_local, preferred_element_type=jnp.float32
    ).astype(jnp.bfloat16)
    values_part = jnp.einsum(
        "nc,chd->nhd", pieces[0], value_local, preferred_element_type=jnp.float32
    ).astype(jnp.bfloat16)
    row_max = jnp.full((heads_dev, tok_rows), -1e30, jnp.float32)
    scores = (
        jnp.einsum("qhd,khd->hqk", query_nope, keys_nope, preferred_element_type=jnp.float32)
        + jnp.einsum("qhd,kd->hqk", query_turn, pieces[1], preferred_element_type=jnp.float32)
    ) * score_scale
    new_max = jnp.maximum(row_max, jnp.max(scores, axis=-1))
    weights = jnp.exp(scores - new_max[:, :, None])
    totals = jnp.sum(weights, axis=-1)
    weighted = jnp.einsum(
        "hqk,khd->hqd",
        weights.astype(jnp.bfloat16),
        values_part,
        preferred_element_type=jnp.float32,
    )
    attended = (weighted / totals[:, :, None]).astype(jnp.bfloat16)
    attended = jnp.transpose(attended, (1, 0, 2)).reshape(tok_rows, heads_dev * value_width)
    row_share = tok_rows // lax.axis_size("tp")
    summed = lax.psum_scatter(
        jnp.dot(attended, out_weight, preferred_element_type=jnp.float32).astype(jnp.bfloat16),
        "tp",
        scatter_dimension=0,
        tiled=True,
    ).astype(jnp.float32)
    own_rows = lax.dynamic_slice_in_dim(residual, tp_index * row_share, row_share, 0).astype(
        jnp.float32
    )
    stream_wide = widened(own_rows + rms_norm(widened(summed), post_gain))
    inputs = lax.all_gather(
        rms_norm(stream_wide, pre_gain).astype(jnp.bfloat16), "tp", axis=0, tiled=True
    )
    ff_dev = up_value.shape[1]
    up_joined = jnp.concatenate([up_value, up_gate], axis=1)
    up_whole = lax.all_gather(up_joined, "sp", axis=0, tiled=True)
    up_pair = jnp.dot(inputs, up_whole, preferred_element_type=jnp.float32).astype(jnp.bfloat16)
    padded = extended(up_pair, (("sp", 0),), 1).astype(jnp.float32)
    channel_start = tp_index * ff_dev
    conv_taps = jnp.concatenate(
        [
            lax.dynamic_slice_in_dim(conv_value, channel_start, ff_dev, 1),
            lax.dynamic_slice_in_dim(conv_gate, channel_start, ff_dev, 1),
        ],
        axis=1,
    ).astype(jnp.float32)
    mixed_conv = (
        padded[:-2] * conv_taps[0] + padded[1:-1] * conv_taps[1] + padded[2:] * conv_taps[2]
    )
    hidden = (jax.nn.silu(mixed_conv[:, ff_dev:]) * mixed_conv[:, :ff_dev]).astype(jnp.bfloat16)
    down_whole = lax.all_gather(down_weight, "sp", axis=1, tiled=True)
    down_terms = jnp.dot(hidden, down_whole, preferred_element_type=jnp.float32)
    reduced = lax.psum_scatter(
        down_terms.astype(jnp.bfloat16), "tp", scatter_dimension=0, tiled=True
    ).astype(jnp.float32)
    return (stream_wide + rms_norm(widened(reduced), ffn_gain)).astype(jnp.bfloat16)


def prep_kernel(latent_ref, rope_ref, gain_ref, cos_ref, sin_ref, turn_ref, out_ref):
    half = out_ref.shape[0]
    first = pl.multiple_of(lax.axis_index("tp") * half, half)
    latent = latent_ref[pl.ds(first, half), :].astype(F32)
    mean = jnp.mean(latent * latent, axis=-1, keepdims=True)
    normed = latent * lax.rsqrt(mean + epsilon) * gain_ref[...].astype(F32)
    width = latent.shape[1]
    out_ref[:, :width] = normed.astype(BF16)
    rope = rope_ref[pl.ds(first, half), :]
    out_ref[:, width:] = turned(rope, cos_ref, sin_ref, turn_ref).astype(BF16)


def turned(vectors, cos_ref, sin_ref, turn_ref):
    swapped = jnp.dot(vectors, turn_ref[...], preferred_element_type=F32)
    return vectors.astype(F32) * cos_ref[...] + swapped * sin_ref[...]


def attend_kernel(
    query_own, query_other, latent_own, latent_other, cos_ref, sin_ref, turn_ref, key_up, value_up,
    out_own, out_other, residual, post_gain, pre_gain, stream_out, inputs_out, queries, mixed,
):
    core = lax.axis_index("tp")
    heads_dev, half, nope = query_own.shape[0], query_own.shape[1], key_up.shape[1] // (2 * query_own.shape[0])
    value_width = value_up.shape[1] // (2 * heads_dev)
    kv = key_up.shape[0]
    rope = query_own.shape[2] - nope
    scale = (nope + rope) ** -0.5 * LOG2E
    own_first, other_first = core * heads_dev, (1 - core) * heads_dev
    for side, (query, first) in enumerate(((query_own, own_first), (query_other, other_first))):
        for h in range(heads_dev):
            rows = pl.ds((side * heads_dev + h) * half, half)
            columns = pl.ds(pl.multiple_of((first + h) * nope, nope), nope)
            absorbed = lax.dot_general(
                query[h, :, :nope], key_up[:, columns], (((1,), (1,)), ((), ())), preferred_element_type=F32
            )
            queries[rows, :kv] = (absorbed * scale).astype(BF16)
            rotated = turned(query[h, :, nope:], cos_ref, sin_ref, turn_ref)
            queries[rows, kv:] = (rotated * scale).astype(BF16)

    block = min(ATTEND_ROWS, queries.shape[0])

    def attend(i, carry):
        rows = pl.ds(pl.multiple_of(i * block, block), block)
        query = queries[rows, :]
        sides = [
            lax.dot_general(query, latent[...], (((1,), (1,)), ((), ())), preferred_element_type=F32)
            for latent in (latent_own, latent_other)
        ]
        top = jnp.maximum(*(jnp.max(s, axis=-1, keepdims=True) for s in sides))
        total, weighted = 0.0, 0.0
        for scores, latent in zip(sides, (latent_own, latent_other)):
            weights = jnp.exp2(scores - top)
            total = total + jnp.sum(weights, axis=-1, keepdims=True)
            weighted = weighted + jnp.dot(weights.astype(BF16), latent[:, :kv], preferred_element_type=F32)
        mixed[rows, :] = (weighted / total).astype(BF16)
        return carry

    lax.fori_loop(0, queries.shape[0] // block, attend, 0)
    summed = 0.0
    for side, (out_weight, first) in enumerate(((out_own, own_first), (out_other, other_first))):
        pieces = []
        for h in range(heads_dev):
            rows = pl.ds((side * heads_dev + h) * half, half)
            columns = pl.ds(pl.multiple_of((first + h) * value_width, value_width), value_width)
            pieces.append(jnp.dot(mixed[rows, :], value_up[:, columns], preferred_element_type=F32).astype(BF16))
        summed = summed + jnp.dot(jnp.concatenate(pieces, axis=1), out_weight[...], preferred_element_type=F32)
    summed = summed.astype(BF16).astype(F32)
    own = residual[pl.ds(pl.multiple_of(core * half, half), half), :].astype(F32)
    mean = jnp.mean(summed * summed, axis=-1, keepdims=True)
    stream = (own + summed * lax.rsqrt(mean + epsilon) * post_gain[...].astype(F32)).astype(BF16)
    stream_out[...] = stream
    wide = stream.astype(F32)
    mean = jnp.mean(wide * wide, axis=-1, keepdims=True)
    inputs_out[...] = (wide * lax.rsqrt(mean + epsilon) * pre_gain[...].astype(F32)).astype(BF16)


def up_kernel(rows_own, rows_other, *refs):
    *weights, out_ref, arranged = refs
    core = lax.axis_index("tp")
    group = lax.axis_index("y") * 2 + lax.axis_index("x")
    blocks, half = rows_own.shape[0], rows_own.shape[1]
    depth = weights[0].shape[1]
    for b in range(blocks):
        for side, rows in ((core, rows_own), (1 - core, rows_other)):
            arranged[pl.ds(pl.multiple_of(b * 2 * half + side * half, half), half), :] = rows[b]
    pieces = []
    for k, z_first, ref in spread(weights, blocks):
        column = [((z_first + z) * 4 + jnp.bitwise_xor(group, k)) * depth for z in range(ref.shape[0])]
        pieces.append((jnp.concatenate([arranged[:, pl.ds(pl.multiple_of(c, depth), depth)] for c in column], axis=1), ref))
    width = out_ref.shape[-1]
    for lo in range(0, width, 256):
        hi = min(lo + 256, width)
        total = 0.0
        for left, ref in pieces:
            right = ref[:, :, lo:hi].reshape(-1, hi - lo)
            total = total + jnp.dot(left, right, preferred_element_type=F32)
        out_ref[:, lo:hi] = total.astype(BF16)


def spread(weights, blocks):
    own, by_x, by_y, low, high = weights
    return ((0, 0, own), (1, 0, by_x), (2, 0, by_y), (3, 0, low), (3, blocks // 2, high))


def down_kernel(rows_ref, before_ref, after_ref, taps_ref, *refs):
    *weights, out_ref, hidden = refs
    group = lax.axis_index("y") * 2 + lax.axis_index("x")
    blocks = before_ref.shape[0]
    length = rows_ref.shape[0] // blocks
    units = hidden.shape[1]
    full = units // 128 * 128

    def mixed(b, lo, hi):
        rows = rows_ref[b * length : (b + 1) * length, lo:hi].astype(F32)
        place = lax.broadcasted_iota(jnp.int32, (length, 1), 0)
        back = jnp.where(place == 0, before_ref[b, :, lo:hi].astype(F32), pltpu.roll(rows, 1, 0))
        ahead = jnp.where(place == length - 1, after_ref[b, :, lo:hi].astype(F32), pltpu.roll(rows, length - 1, 0))
        return back * taps_ref[0:1, lo:hi] + rows * taps_ref[1:2, lo:hi] + ahead * taps_ref[2:3, lo:hi]

    for b in range(blocks):
        rows = slice(b * length, (b + 1) * length)
        for lo in range(0, full, 128):
            gate = mixed(b, full + lo, full + lo + 128)
            hidden[rows, lo : lo + 128] = (gate / (1.0 + jnp.exp(-gate)) * mixed(b, lo, lo + 128)).astype(BF16)
        if units > full:
            both = mixed(b, 2 * full, 2 * units)
            gate, value = both[:, units - full :], both[:, : units - full]
            hidden[rows, full:] = (gate / (1.0 + jnp.exp(-gate)) * value).astype(BF16)
    left = hidden[...]
    for k, z_first, ref in spread(weights, blocks):
        for z in range(0, ref.shape[0], 2):
            right = jnp.concatenate([ref[z], ref[z + 1]], axis=1)
            part = jnp.dot(left, right, preferred_element_type=F32).astype(BF16)
            width = ref.shape[2]
            for i in range(2):
                column = ((z_first + z + i) * 4 + jnp.bitwise_xor(group, k)) * width
                out_ref[:, pl.ds(pl.multiple_of(column, width), width)] = part[:, i * width : (i + 1) * width]


def call(kernel, out_shape, args, scratch=()):
    return pl.pallas_call(
        kernel,
        out_shape=out_shape,
        in_specs=[pl.BlockSpec(memory_space=pltpu.VMEM)] * len(args),
        out_specs=jax.tree.map(lambda _: pl.BlockSpec(memory_space=pltpu.VMEM), out_shape),
        scratch_shapes=list(scratch),
        compiler_params=pltpu.CompilerParams(vmem_limit_bytes=56 * 2**20),
    )(*args)


def swap(x, axis):
    return lax.ppermute(x, axis, [(0, 1), (1, 0)])


def shift(x, axis, by):
    size = lax.axis_size(axis)
    return lax.ppermute(x, axis, [(i, (i + by) % size) for i in range(size)])


def after(x, *others):
    return lax.optimization_barrier((x, *others))[0]


def exchanged(x):
    return lax.all_to_all(x, "c", split_axis=0, concat_axis=0, tiled=True)


def spread_out(own):
    cut = own.shape[0] // 2
    by_x, by_y = swap(own, "x"), swap(own, "y")
    return own, by_x, by_y, swap(by_x[:cut], "y"), swap(by_y[cut:], "x")


def fast_body(
    residual, query_nope, query_rope, latent, rope_key, kv_gain, key_up, value_up, out_weight, post_gain,
    pre_gain, ffn_gain, up_value, up_gate, conv_value, conv_gate, down_weight,
):
    tok_rows, model = residual.shape
    half = tok_rows // 2
    heads_dev = query_nope.shape[1]
    core = lax.axis_index("tp")
    group = lax.axis_index("y") * 2 + lax.axis_index("x")
    place = lax.axis_index("c")
    n_c = lax.axis_size("c")
    shape = jax.ShapeDtypeStruct

    rope = rope_key.shape[1]
    pairs = rope // 4
    frequency = rope_base ** (-np.arange(pairs) / pairs)
    grid_rows = tok_rows * n_c * 4 // GRID
    row_angle = np.arange(grid_rows)[:, None] * frequency
    column_angle = np.arange(GRID)[:, None] * frequency
    grid_row = (place * 4 + group) * 2 + core

    def table(fn, sign):
        row = np.concatenate([sign * fn(row_angle), fn(row_angle)], axis=1).astype(np.float32)
        column = np.concatenate([sign * fn(column_angle), fn(column_angle)], axis=1).astype(np.float32)
        row = lax.dynamic_slice_in_dim(jnp.asarray(row), grid_row, 1, 0)
        return jnp.concatenate([jnp.broadcast_to(row, column.shape), jnp.asarray(column)], axis=1)

    cosine, sine = table(np.cos, 1.0), table(np.sin, -1.0)
    turn = np.zeros((rope, rope), np.float32)
    for j in range(rope):
        turn[j ^ pairs, j] = 1.0
    turn = jnp.asarray(turn, BF16)

    prepared = call(
        prep_kernel,
        shape((half, latent.shape[1] + rope), BF16),
        (latent, rope_key, kv_gain[None], cosine, sine, turn),
    )
    rings = jnp.stack([prepared] + [shift(prepared, "c", d) for d in range(1, n_c)])

    units = up_value.shape[1] // n_c
    full = units // 128 * 128

    def joined(value, gate):
        v, g = (w.reshape(w.shape[0], n_c, units) for w in (value, gate))
        return jnp.concatenate([v[..., :full], g[..., :full], v[..., full:], g[..., full:]], axis=2)

    up_pieces = jnp.transpose(joined(up_value, up_gate), (1, 0, 2))
    down_pieces = down_weight.reshape(n_c, units, down_weight.shape[1])
    up_own = exchanged(after(up_pieces, rings))
    up_parts = spread_out(up_own)
    down_own = exchanged(after(down_pieces, rings))
    down_parts = spread_out(down_own)

    query = jnp.transpose(jnp.concatenate([query_nope, query_rope], axis=2), (1, 0, 2))
    query_own = lax.dynamic_slice_in_dim(query, core * half, half, 1)
    query_other = swap(lax.dynamic_slice_in_dim(query, (1 - core) * half, half, 1), "tp")
    out_other = swap(out_weight, "tp")

    by_x, by_y = swap(rings, "x"), swap(rings, "y")
    across = lax.ppermute(rings, ("y", "x"), [(0, 3), (3, 0), (1, 2), (2, 1)])
    latent_own = jnp.concatenate([rings, by_x, by_y, across]).reshape(-1, rings.shape[-1])
    latent_other = swap(latent_own, "tp")

    stream, inputs = call(
        attend_kernel,
        (shape((half, model), BF16), shape((half, model), BF16)),
        (
            query_own, query_other, latent_own, latent_other, cosine, sine, turn,
            key_up.reshape(key_up.shape[0], -1), value_up.reshape(value_up.shape[0], -1),
            out_weight, out_other, residual, post_gain[None], pre_gain[None],
        ),
        [
            pltpu.VMEM((2 * heads_dev * half, latent_own.shape[1]), BF16),
            pltpu.VMEM((2 * heads_dev * half, latent.shape[1]), BF16),
        ],
    )

    rows_own = jnp.stack([inputs] + [shift(inputs, "c", d) for d in range(1, n_c)])
    rows_other = swap(rows_own, "tp")
    up_rows = call(
        up_kernel,
        shape((n_c * tok_rows, 2 * units), BF16),
        (rows_own, rows_other, *up_parts),
        [pltpu.VMEM((n_c * tok_rows, model), BF16)],
    )
    edges = up_rows.reshape(n_c, tok_rows, 2 * units)
    before = shift(edges[:, -1:], ("y", "x"), 1)
    following = shift(edges[:, :1], ("y", "x"), -1)
    block = (place - jnp.arange(n_c)) % n_c
    before_turn = jnp.where((block == 0)[:, None, None], 0, jnp.roll(before, -1, 0))
    before = jnp.where(group == 0, before_turn, before)
    following_turn = jnp.where((block == n_c - 1)[:, None, None], 0, jnp.roll(following, 1, 0))
    following = jnp.where(group == 3, following_turn, following)
    start = (core * n_c + place) * units
    value_taps, gate_taps = (lax.dynamic_slice_in_dim(w, start, units, 1) for w in (conv_value, conv_gate))
    taps = jnp.concatenate(
        [value_taps[:, :full], gate_taps[:, :full], value_taps[:, full:], gate_taps[:, full:]], axis=1
    ).astype(F32)
    partial = call(
        down_kernel,
        shape((n_c * tok_rows, model), BF16),
        (up_rows, before, following, taps, *down_parts),
        [pltpu.VMEM((n_c * tok_rows, units), BF16)],
    ).reshape(n_c, 2, half, model)
    kept = lax.dynamic_index_in_dim(partial, core, 1, keepdims=False)
    given = swap(lax.dynamic_index_in_dim(partial, 1 - core, 1, keepdims=False), "tp")
    sums = (kept.astype(F32) + given.astype(F32)).astype(BF16)
    projected = sums[0].astype(F32)
    for d in range(1, n_c):
        projected = projected + shift(sums[d], "c", -d).astype(F32)
    return (stream.astype(F32) + rms_norm(widened(projected), ffn_gain)).astype(BF16)


def placed(sp):
    return (
        P(sp, None),
        P(sp, "tp", None),
        P(sp, "tp", None),
        P(sp, None),
        P(sp, None),
        P(),
        P(),
        P(),
        P("tp", None),
        P(),
        P(),
        P(),
        P(sp, "tp"),
        P(sp, "tp"),
        P(),
        P(),
        P("tp", sp),
    )


def solution(mesh):
    def mapped(fn, on, sp):
        out = P((*sp, "tp") if isinstance(sp, tuple) else (sp, "tp"), None)
        return jax.shard_map(fn, mesh=on, in_specs=placed(sp), out_specs=out, check_vma=False)

    sp, tp = mesh.shape["sp"], mesh.shape["tp"]

    def step(*args):
        tokens, units, model = args[0].shape[0], args[12].shape[1], args[0].shape[1]
        fits = tp == 2 and sp % 8 == 0 and tokens == 2 * sp * GRID and model % (128 * sp) == 0
        if not fits or units % (tp * sp // 4 * 64) or units // (tp * sp // 4) < 128:
            return mapped(body, mesh, "sp")(*args)
        fine = Mesh(mesh.devices.reshape(sp // 4, 2, 2, tp), ("c", "y", "x", "tp"))
        return mapped(fast_body, fine, ("c", "y", "x"))(*args)

    return step
```
